32 devices in a mesh: ep: 8 (over z, x), tp: 4 (over y, core).
Axes of the slice: x: 2, y: 2, z: 4, core: 2. Of those that a mesh axis runs over, the one named last changes fastest.
Arguments:
- mixer_input: bfloat16 [1024, 2048], P('ep'), may hold values from -6 to 6
- mixer_gain: float32 [2048], replicated, may hold values from 0.1 to 1.9
- query_weight: bfloat16 [2048, 2048], P(None, 'tp'), may hold values from -0.125 to 0.125
- key_weight: bfloat16 [2048, 2048], P(None, 'tp'), may hold values from -0.125 to 0.125
- value_weight: bfloat16 [2048, 2048], P(None, 'tp'), may hold values from -0.125 to 0.125
- score_offset: float32 [16], P('tp'), may hold values from -8.6 to -4
- out_weight: bfloat16 [2048, 2048], P(None, 'tp'), may hold values from -1.3203125 to 1.3203125
- expert_input: bfloat16 [1024, 2048], P('ep'), may hold values from -6 to 6
- expert_gain: float32 [2048], replicated, may hold values from 0.1 to 1.9
- route_ids: int32 [1024, 2], P('ep'), may hold values from 0 to 7, as said below
- route_weights: float32 [1024, 2], P('ep'), may hold values from 0.1 to 1
- gate_weight: bfloat16 [8, 2048, 2048], P('ep', None, 'tp'), may hold values from -0.125 to 0.125
- up_weight: bfloat16 [8, 2048, 2048], P('ep', None, 'tp'), may hold values from -0.125 to 0.125
- down_weight: bfloat16 [8, 2048, 2048], P('ep', 'tp'), may hold values from -0.1875 to 0.1875
Outputs:
- mixer_output: bfloat16 [1024, 2048], P('ep', 'tp')
- expert_output: bfloat16 [1024, 2048], P('ep', 'tp')
The draws below stay inside these ranges and needn't reach their ends.
Inputs may be any that keep to these rules, and one draw needn't show every extreme that they name: `route_ids`: each row names two different experts of one group; group g holds experts g * 2 to g * 2 + 1. Among the rows of one ep index no expert is named more than 64 times, and in every draw the experts of some group are each named exactly 64 times by the rows of every ep index.
All inputs are finite; a program needn't handle non-finite values.
Results may differ from the reference program's by a relative error of at most 0.019.
Values may be sent and summed in bfloat16 or wider, within the bound.
A program may use at most 64 MiB of HBM per device.

```python
import jax
import jax.numpy as jnp
from jax import lax

D = 2048
HEADS = 16
HD = 128
SUB = 64
FF = 2048
GROUPS = 4
TOK_A = 128
TOK_B = 128
EXPERTS = 8
CAP = 64
TOKENS_A = 1024
TOKENS_B = 1024
N_EP = 8
N_TP = 4


def draw_score_offset(key, part):
    return jax.random.uniform(key, (HEADS,), jnp.float32, -8.6, -4.0)


def draw_route_ids(key, part):
    group_count = GROUPS
    per_group = EXPERTS // GROUPS
    block_count = TOKENS_B // TOK_B
    key_busy, key_perm, key_rot = jax.random.split(jax.random.fold_in(key, 7), 3)
    busy = jax.random.randint(key_busy, (), 0, group_count)
    ranks = jax.vmap(lambda sub_key: jax.random.permutation(sub_key, TOK_B))(jax.random.split(key_perm, block_count)).astype(jnp.int32)
    half_rows = TOK_B // 2
    heavy = ranks < half_rows
    others = ranks - half_rows
    group_id = jnp.where(heavy, busy, (busy + 1 + others % (group_count - 1)) % group_count)
    within_rank = jnp.where(heavy, ranks, others // (group_count - 1))
    rotation = jax.random.randint(key_rot, (block_count, group_count), 0, per_group)
    row_rotation = jnp.take_along_axis(rotation, group_id, axis=1)
    first_pick = (within_rank % per_group + row_rotation) % per_group
    step_size = max(per_group - 1, 1)
    second_pick = (within_rank % per_group + 1 + within_rank // per_group % step_size + row_rotation) % per_group
    both = jnp.stack([group_id * per_group + first_pick, group_id * per_group + second_pick], axis=-1)
    return both.reshape(TOKENS_B, 2).astype(jnp.int32)


def with_spikes(drawn, own_key, source, target, parts, factor):
    def block_of(axis_at):
        return (jnp.arange(drawn.shape[axis_at]) // (drawn.shape[axis_at] // parts)).reshape((-1,) + (1,) * (drawn.ndim - 1 - axis_at))

    one_side = jax.random.permutation(own_key, parts)[block_of(target)]
    far = (block_of(target) + parts // 2) % parts
    return jnp.where((block_of(source) == one_side) | (block_of(source) == far), factor * drawn, drawn)


def block_scale(key, dims, shards, least, high):
    def one(axis_at, blocks):
        steps = jax.random.uniform(jax.random.fold_in(jax.random.fold_in(key, 6), axis_at), (blocks,), jnp.float32, least / len(shards), high / len(shards))
        return jnp.repeat(jnp.exp(steps), dims[axis_at] // blocks).reshape((-1,) + (1,) * (len(dims) - axis_at - 1))

    level = one(*shards[0])
    for cut in shards[1:]:
        level = level * one(*cut)
    return level


def centred(rng, shape, deviation, limit, shards=(), kind=jnp.bfloat16):
    array = jax.random.normal(rng, shape, jnp.float32) * deviation
    if len(shards) > 0:
        array = block_scale(rng, shape, shards, -0.22, 0.18) * array
    return jnp.clip(array, min=-limit, max=limit).astype(kind)


def bell_draw_with(stream_key, dims, width, limit, pieces, heavy, kind=jnp.bfloat16):
    values = width * jax.random.normal(stream_key, dims, jnp.float32)
    if pieces:
        values = values * block_scale(stream_key, dims, pieces, -0.22, 0.18)
    return jnp.clip(with_spikes(values, jax.random.fold_in(stream_key, 3), *heavy), -limit, limit).astype(kind)


def setup_inputs(seed: int = 0) -> dict:
    seeds = jax.random.split(jax.random.key(seed), 15)
    mixer_input = centred(seeds[0], (TOKENS_A, D), 1.0, 6.0, ((0, 8),))
    mixer_gain = jnp.clip(1.0 + 0.18 * jax.random.normal(seeds[1], (D,), jnp.float32), 0.1, 1.9)
    query_weight = centred(seeds[2], (D, HEADS * HD), D ** -0.5, 0.125, ((1, 4),))
    key_weight = centred(seeds[3], (D, HEADS * HD), D ** -0.5, 0.125, ((1, 4),))
    value_weight = centred(seeds[4], (D, HEADS * HD), D ** -0.5, 0.125, ((1, 4),))
    score_offset = draw_score_offset(jax.random.fold_in(seeds[14], 71), 0)
    out_weight = centred(seeds[6], (HEADS * HD, D), (10 * (HEADS * HD) ** -0.5), 1.3203125, ((1, 4),))
    expert_input = centred(seeds[7], (TOKENS_B, D), 1.0, 6.0, ((0, 8),))
    expert_gain = jnp.clip(1.0 + 0.18 * jax.random.normal(seeds[8], (D,), jnp.float32), 0.1, 1.9)
    route_ids = draw_route_ids(jax.random.fold_in(seeds[14], 71), 0)
    route_weights = jnp.clip(0.1 + 0.9 * jax.random.uniform(seeds[10], (TOKENS_B, 2), jnp.float32) ** block_scale(seeds[10], (TOKENS_B, 2), ((0, 8),), -0.2, 0.2), 0.1, 1.0)
    gate_weight = centred(seeds[11], (EXPERTS, D, FF), D ** -0.5, 0.125, ((0, 8), (2, 4)))
    up_weight = centred(seeds[12], (EXPERTS, D, FF), D ** -0.5, 0.125, ((0, 8), (2, 4)))
    down_weight = bell_draw_with(seeds[13], (EXPERTS, FF, D), FF ** -0.5, 0.1875, ((0, 8), (1, 4)), (1, 2, 4, 2.0))
    return {"mixer_input": mixer_input, "mixer_gain": mixer_gain, "query_weight": query_weight, "key_weight": key_weight, "value_weight": value_weight, "score_offset": score_offset, "out_weight": out_weight, "expert_input": expert_input, "expert_gain": expert_gain, "route_ids": route_ids, "route_weights": route_weights, "gate_weight": gate_weight, "up_weight": up_weight, "down_weight": down_weight}


epsilon = 1e-06

def rms_rows(rows_in, gain):
    values_f = rows_in.astype(jnp.float32)
    scaled = values_f * lax.rsqrt(lax.optimization_barrier(jnp.mean(values_f * values_f, axis=-1, keepdims=True)) + epsilon)
    return (scaled * gain).astype(jnp.bfloat16)

def key_block(query_blk, key_blk, value_blk, score_offset, query_start, key_start):
    head_count, query_len, head_size = query_blk.shape
    key_len = key_blk.shape[1]
    scores = jnp.einsum('hqd,hkd->hqk', query_blk.astype(jnp.float32), key_blk.astype(jnp.float32))
    scores = scores * head_size ** (-0.5) + score_offset[:, None, None]
    query_pos = query_start + jnp.arange(query_len, dtype=jnp.int32)
    key_pos = key_start + jnp.arange(key_len, dtype=jnp.int32)
    causal = (key_pos[None, :] < query_pos[:, None])[None]
    log_keep = jnp.where(causal, jax.nn.log_sigmoid(-scores), 0.0)
    suffix_ones = jnp.tril(jnp.ones((SUB, SUB), jnp.float32))
    within = jnp.einsum('hqns,sr->hqnr', log_keep.reshape(head_count, query_len, key_len // SUB, SUB), suffix_ones, precision=lax.Precision.HIGHEST)
    sub_total = within[..., 0]
    later_subs = lax.cumsum(sub_total, axis=2, reverse=True) - sub_total
    after_sum = (within + later_subs[..., None]).reshape(head_count, query_len, key_len) - log_keep
    weights = jnp.where(causal, jnp.exp(jax.nn.log_sigmoid(scores) + after_sum), 0.0).astype(jnp.bfloat16)
    block_part = jnp.einsum('hqk,hkd->hqd', weights.astype(jnp.float32), value_blk.astype(jnp.float32))
    return (block_part, lax.optimization_barrier(jnp.sum(sub_total, axis=2)))

def attention_half(mixer_input, mixer_gain, query_weight, key_weight, value_weight, score_offset, out_weight):
    normed = rms_rows(mixer_input, mixer_gain)

    def project(weight):
        made = jnp.dot(normed, weight, preferred_element_type=jnp.float32).astype(jnp.bfloat16)
        return made.reshape(TOKENS_A, HEADS, HD).transpose(1, 0, 2)
    queries = project(query_weight)
    key_all = project(key_weight)
    value_all = project(value_weight)

    def query_block(block_idx):
        query_blk = lax.dynamic_slice_in_dim(queries, block_idx * TOK_A, TOK_A, 1)

        def step(turn, carried):
            running, keep_sum = carried
            key_idx = block_idx - turn
            key_blk = lax.dynamic_slice_in_dim(key_all, key_idx * TOK_A, TOK_A, 1)
            value_blk = lax.dynamic_slice_in_dim(value_all, key_idx * TOK_A, TOK_A, 1)
            block_part, block_keep = key_block(query_blk, key_blk, value_blk, score_offset, block_idx * TOK_A, key_idx * TOK_A)
            return (running + jnp.exp(keep_sum)[..., None] * block_part, keep_sum + block_keep)
        initial = (jnp.zeros((HEADS, TOK_A, HD), jnp.float32), jnp.zeros((HEADS, TOK_A), jnp.float32))
        running, unused = lax.fori_loop(0, block_idx + 1, step, initial)
        return running.astype(jnp.bfloat16)
    blocks = lax.map(query_block, jnp.arange(N_EP, dtype=jnp.int32))
    attended = blocks.transpose(0, 2, 1, 3).reshape(TOKENS_A, HEADS * HD)
    return jnp.dot(attended, out_weight, preferred_element_type=jnp.float32).astype(jnp.bfloat16)

def expert_half(expert_input, expert_gain, route_ids, route_weights, gate_weight, up_weight, down_weight):
    normed = rms_rows(expert_input, expert_gain)
    flat_ids = route_ids.reshape(-1)
    assigns = TOKENS_B * 2
    rows_max = N_EP * CAP
    padded = jnp.concatenate([normed, jnp.zeros((1, D), jnp.bfloat16)], axis=0)

    def one_expert(gathered, expert_idx):
        chosen = jnp.nonzero(flat_ids == expert_idx, size=rows_max, fill_value=assigns)[0].astype(jnp.int32)
        row_idx = jnp.minimum(chosen // 2, TOKENS_B).astype(jnp.int32)
        rows_in = padded[row_idx]
        gate_sum = jnp.dot(rows_in, gate_weight[expert_idx], preferred_element_type=jnp.float32)
        up_sum = jnp.dot(rows_in, up_weight[expert_idx], preferred_element_type=jnp.float32)
        hidden = (jax.nn.silu(gate_sum) * up_sum).astype(jnp.bfloat16)
        partial_out = jnp.einsum('rtf,tfd->trd', hidden.reshape(rows_max, N_TP, FF // N_TP).astype(jnp.float32), down_weight[expert_idx].reshape(N_TP, FF // N_TP, D).astype(jnp.float32))
        rounded = lax.optimization_barrier(partial_out.astype(jnp.bfloat16))
        result = lax.optimization_barrier(jnp.sum(rounded.astype(jnp.float32), axis=0)).astype(jnp.bfloat16)
        return (gathered.at[chosen].set(result, mode='drop'), None)
    gathered, unused = lax.scan(one_expert, jnp.zeros((assigns, D), jnp.bfloat16), jnp.arange(EXPERTS, dtype=jnp.int32))
    mixed_rows = route_weights[:, :, None] * gathered.reshape(TOKENS_B, 2, D).astype(jnp.float32)
    return lax.optimization_barrier(jnp.sum(mixed_rows, axis=1)).astype(jnp.bfloat16)

def reference(mixer_input, mixer_gain, query_weight, key_weight, value_weight, score_offset, out_weight, expert_input, expert_gain, route_ids, route_weights, gate_weight, up_weight, down_weight):
    mixer_output = attention_half(mixer_input, mixer_gain, query_weight, key_weight, value_weight, score_offset, out_weight)
    expert_output = expert_half(expert_input, expert_gain, route_ids, route_weights, gate_weight, up_weight, down_weight)
    return (mixer_output, expert_output)
```

```python
import functools
import math

import jax
import jax.numpy as jnp
from jax import lax
from jax.experimental import pallas as pl
from jax.experimental.pallas import tpu as pltpu
from jax.sharding import PartitionSpec as P

HD = 128
SUB = 64
GROUPS = 4


epsilon = 1e-06


def rms_rows(rows_in, gain):
    values_f = rows_in.astype(jnp.float32)
    scaled = values_f * lax.rsqrt(jnp.mean(values_f * values_f, axis=-1, keepdims=True) + epsilon)
    return (scaled * gain).astype(jnp.bfloat16)


def token_mixer(
    mixer_input, mixer_gain, query_weight, key_weight, value_weight, score_offset, out_weight
):
    rows_here = mixer_input.shape[0]
    normed = rms_rows(mixer_input, mixer_gain)
    queries = jnp.dot(normed, query_weight, preferred_element_type=jnp.float32).astype(jnp.bfloat16)
    key_rows = jnp.dot(normed, key_weight, preferred_element_type=jnp.float32).astype(jnp.bfloat16)
    value_rows = jnp.dot(normed, value_weight, preferred_element_type=jnp.float32).astype(
        jnp.bfloat16
    )
    heads_here = queries.shape[1] // HD
    blocks = lax.axis_size("ep")
    my_block = lax.axis_index("ep")
    suffix_ones = jnp.tril(jnp.ones((SUB, SUB), jnp.float32))
    query_sets = (
        (queries, my_block * rows_here + jnp.arange(rows_here, dtype=jnp.int32), my_block),
    )

    def attend_set(query_flat, query_pos, key_heads, value_heads, shards):
        query_count = query_flat.shape[0]
        query_heads = query_flat.reshape(query_count, heads_here, HD)
        scores = jnp.einsum(
            "qhd,bkhd->bhqk", query_heads, key_heads, preferred_element_type=jnp.float32
        )
        scores = scores * HD ** (-0.5) + score_offset[None, :, None, None]
        key_pos = jnp.arange(shards * rows_here, dtype=jnp.int32).reshape(shards, 1, 1, rows_here)
        causal = key_pos < query_pos.reshape(1, 1, query_count, 1)
        log_keep = jnp.where(causal, jax.nn.log_sigmoid(-scores), 0.0)
        within = jnp.einsum(
            "bhqns,sr->bhqnr",
            log_keep.reshape(shards, heads_here, query_count, rows_here // SUB, SUB),
            suffix_ones,
            precision=lax.Precision.HIGHEST,
        )
        sub_total = within[..., 0]
        later_subs = lax.cumsum(sub_total, axis=3, reverse=True) - sub_total
        after_sum = (within + later_subs[..., None]).reshape(
            shards, heads_here, query_count, rows_here
        ) - log_keep
        weights = jnp.where(causal, jnp.exp(jax.nn.log_sigmoid(scores) + after_sum), 0.0).astype(
            jnp.bfloat16
        )
        block_part = jnp.einsum(
            "bhqk,bkhd->bqhd", weights, value_heads, preferred_element_type=jnp.float32
        )
        keep_part = jnp.sum(sub_total, axis=3).transpose(0, 2, 1)
        return (block_part, keep_part)

    def bind_attend(query_flat, query_pos, key_heads, value_heads, shards):

        def attend(state_in):
            return attend_set(query_flat, query_pos, key_heads, value_heads, shards)

        return attend

    def untouched(state_in):
        return state_in

    initial = tuple(
        (
            (
                jnp.zeros((blocks, entry[0].shape[0], heads_here, HD), jnp.float32),
                jnp.zeros((blocks, entry[0].shape[0], heads_here), jnp.float32),
            )
            for entry in query_sets
        )
    )
    key_part = lax.all_gather(key_rows, "ep", axis=0, tiled=True)
    value_part = lax.all_gather(value_rows, "ep", axis=0, tiled=True)
    shards = key_part.shape[0] // rows_here
    first_block = jnp.int32(0) // rows_here
    key_heads = key_part.reshape(shards, rows_here, heads_here, HD)
    value_heads = value_part.reshape(shards, rows_here, heads_here, HD)
    updated = []
    for (query_flat, query_pos, limit), state_in in zip(query_sets, initial):
        attend = bind_attend(query_flat, query_pos, key_heads, value_heads, shards)
        updated.append(lax.cond(first_block <= limit, attend, untouched, state_in))
    folded = tuple(updated)
    finished = []
    for block_out, block_keep in folded:
        later_keep = lax.cumsum(block_keep, axis=0, reverse=True) - block_keep
        summed = jnp.sum(jnp.exp(later_keep)[..., None] * block_out, axis=0)
        finished.append(summed.astype(jnp.bfloat16).reshape(block_out.shape[1], heads_here * HD))
    attended = finished[0]
    mixed_out = jnp.dot(
        lax.all_gather(attended, "tp", axis=1, tiled=True),
        out_weight,
        preferred_element_type=jnp.float32,
    )
    return mixed_out.astype(jnp.bfloat16)


def finish_expert(gate_sum, up_sum, sources, slot_count, down_weight):
    hidden = (jax.nn.silu(gate_sum) * up_sum).astype(jnp.bfloat16)
    partial_out = jnp.dot(hidden, down_weight[0], preferred_element_type=jnp.float32)
    partial_out = partial_out.reshape(sources, slot_count, partial_out.shape[1])
    summed = lax.psum_scatter(
        partial_out.astype(jnp.bfloat16), "tp", scatter_dimension=2, tiled=True
    )
    return lax.all_to_all(summed, "ep", split_axis=0, concat_axis=0, tiled=True)


def routed_experts(
    expert_input, expert_gain, route_ids, route_weights, gate_weight, up_weight, down_weight
):
    rows_here = expert_input.shape[0]
    model_width = expert_input.shape[1]
    normed = rms_rows(expert_input, expert_gain)
    experts = lax.axis_size("ep")
    capacity = rows_here // (experts // GROUPS)
    flat_ids = route_ids.reshape(-1)
    onehot = (flat_ids[:, None] == jnp.arange(experts, dtype=jnp.int32)[None, :]).astype(jnp.int32)
    slot_index = jnp.sum((jnp.cumsum(onehot, axis=0) - 1) * onehot, axis=1)
    target = flat_ids * capacity + slot_index
    assign_row = jnp.arange(flat_ids.shape[0], dtype=jnp.int32) // 2
    source_row = jnp.full((experts * capacity,), rows_here, jnp.int32).at[target].set(assign_row)
    narrow = model_width // lax.axis_size("tp")
    own_cols = lax.dynamic_slice_in_dim(normed, lax.axis_index("tp") * narrow, narrow, 1)
    padded = jnp.concatenate([own_cols, jnp.zeros((1, narrow), jnp.bfloat16)], axis=0)
    outgoing = padded[source_row].reshape(experts, capacity, narrow)
    arrived = lax.all_to_all(outgoing, "ep", split_axis=0, concat_axis=0, tiled=True)
    row_count = arrived.shape[0] * arrived.shape[1]
    fetched = lax.all_gather(arrived, "tp", axis=2, tiled=True)
    flat_rows = fetched.reshape(row_count, fetched.shape[2])
    gate_rows = gate_weight[0]
    up_rows = up_weight[0]
    gate_sum = jnp.dot(flat_rows, gate_rows, preferred_element_type=jnp.float32)
    up_sum = jnp.dot(flat_rows, up_rows, preferred_element_type=jnp.float32)
    returned = finish_expert(gate_sum, up_sum, arrived.shape[0], arrived.shape[1], down_weight)
    out_cols = returned.shape[2]
    picked = returned.reshape(experts * capacity, out_cols)[target].astype(jnp.float32)
    picked = picked.reshape(rows_here, 2, out_cols)
    combined = jnp.sum(route_weights[:, :, None] * picked, axis=1)
    return combined.astype(jnp.bfloat16)


def on_device(
    mixer_input,
    mixer_gain,
    query_weight,
    key_weight,
    value_weight,
    score_offset,
    out_weight,
    expert_input,
    expert_gain,
    route_ids,
    route_weights,
    gate_weight,
    up_weight,
    down_weight,
):
    mixer_output = token_mixer(
        mixer_input, mixer_gain, query_weight, key_weight, value_weight, score_offset, out_weight
    )
    expert_output = routed_experts(
        expert_input, expert_gain, route_ids, route_weights, gate_weight, up_weight, down_weight
    )
    return (mixer_output, expert_output)


class Wires:
    def __init__(self, send_sem, recv_sems):
        self.send_sem = send_sem
        self.recv_sems = recv_sems
        self.sent_bytes = 0
        self.used = 0

    def take(self, count):
        first = self.used
        self.used += count
        return first

    def send(self, src, dst, slot, peer, lane=0):
        if lane == 0:
            self.sent_bytes += math.prod(src.shape) * 2
        pltpu.make_async_remote_copy(
            src_ref=src,
            dst_ref=dst,
            send_sem=self.send_sem.at[lane],
            recv_sem=self.recv_sems.at[slot],
            device_id=peer,
            device_id_type=pl.DeviceIdType.MESH,
        ).start()

    def arrived(self, like, slot):
        pltpu.make_async_copy(like, like, self.recv_sems.at[slot]).wait()

    def drain(self, like):
        row_bytes = like.shape[1] * 2
        whole = like.at[pl.ds(0, self.sent_bytes // row_bytes), :]
        pltpu.make_async_copy(whole, whole, self.send_sem.at[0]).wait()


WIRES = 56
LOADS = 14


def fused_kernel(
    groups,
    xa_hbm, ga_hbm, wq_hbm, wk_hbm, wv_hbm, off_hbm, wo_hbm,
    xb_hbm, gb_hbm, ids_hbm, rw_hbm, gate_hbm, up_hbm, down_hbm,
    out_ref,
    xa_ref, ga_ref, off_ref, xb_ref, gb_ref, ids_ref, rw_ref,
    weights, down, load_sems,
    nb, pick, sendb, sendw, rows_all, wt_all, wt_col,
    kv_s, q_s, kv_all, q_all, acc, att_s, att,
    hid, give, core_in, keep_f, s1, first_in, mid_in, s2, final, back,
    send_sem, recv_sems,
):
    f32, bf16 = jnp.float32, jnp.bfloat16
    e = lax.axis_index("ep")
    t = lax.axis_index("tp")
    z = lax.div(e, 2)
    x = lax.rem(e, 2)
    rows, width = xb_ref.shape
    cap = rows // 2
    mix_ref, exp_ref = out_ref.at[0], out_ref.at[1]
    narrow = mix_ref.shape[1]
    pool = groups * cap
    tc = t + 1 - 2 * lax.rem(t, 2)
    ty = lax.rem(t + 2, 4)
    tyc = lax.rem(tc + 2, 4)
    across = {"ep": e + 1 - 2 * x, "tp": t}
    side = {"ep": e, "tp": ty}
    twin = {"ep": e, "tp": tc}

    def peer(step, other):
        xx = 1 - x if other else x
        return {"ep": 2 * lax.rem(z + step, groups) + xx, "tp": t}

    def zfrom(step):
        return lax.rem(z + groups - step, groups)

    def zto(step):
        return lax.rem(z + step, groups)

    barrier = pltpu.get_barrier_semaphore()
    greeted = [side, twin] + [
        peer(step, other) for step in range(groups) for other in (0, 1) if step or other
    ]
    for device in greeted:
        pl.semaphore_signal(barrier, inc=1, device_id=device, device_id_type=pl.DeviceIdType.MESH)

    def weight(k):
        return weights.at[pl.ds(k * width, width), :]

    wk, wv, wq, gate, up, wo = (weight(k) for k in range(6))
    loads = {}
    for slot, (name, from_hbm, to) in enumerate((
        ("xb", xb_hbm, xb_ref), ("ids", ids_hbm, ids_ref), ("gb", gb_hbm, gb_ref), ("rw", rw_hbm, rw_ref),
        ("xa", xa_hbm, xa_ref), ("ga", ga_hbm, ga_ref), ("wk", wk_hbm, wk), ("wv", wv_hbm, wv),
        ("wq", wq_hbm, wq), ("gate", gate_hbm.at[0], gate), ("up", up_hbm.at[0], up),
        ("down", down_hbm.at[0], down), ("wo", wo_hbm, wo), ("off", off_hbm, off_ref),
    )):
        loads[name] = pltpu.make_async_copy(from_hbm, to, load_sems.at[slot])
        loads[name].start()

    def norm(in_ref, gain_ref):
        vals = in_ref[...].astype(f32)
        scale = lax.rsqrt(jnp.mean(vals * vals, axis=-1, keepdims=True) + epsilon)
        return (vals * scale * gain_ref[...]).astype(bf16)

    loads["ids"].wait()
    lane = lax.broadcasted_iota(jnp.int32, (rows, rows), 1)
    row = lax.broadcasted_iota(jnp.int32, (rows, rows), 0)
    id_row = jnp.broadcast_to(ids_ref[0:1, :].astype(f32), (rows, rows))
    id0 = jnp.transpose(id_row).astype(jnp.int32)
    id_row = id_row.astype(jnp.int32)
    grp = lax.div(id0, jnp.full_like(id0, 2))
    odd = (id_row - 2 * lax.div(id_row, jnp.full_like(id_row, 2))) == 1
    onehot = jnp.where(lane == grp, 1.0, 0.0)
    before = jnp.where(lane < row, 1.0, 0.0)
    count = jnp.dot(before.astype(bf16), onehot.astype(bf16), preferred_element_type=f32)
    place = jnp.sum(count * onehot, axis=1, keepdims=True)
    grp_f = grp[:, 0:1].astype(f32)
    target = grp_f * cap + place
    slots = lax.broadcasted_iota(jnp.int32, (rows, pool), 1).astype(f32)
    chosen = jnp.where(slots == target, 1.0, 0.0)
    pick[...] = chosen.astype(bf16)
    turned = jnp.transpose(chosen).astype(bf16)
    loads["xb"].wait()
    loads["gb"].wait()
    nb[...] = norm(xb_ref, gb_ref)
    my_cols = pl.ds(pl.multiple_of(t * narrow, 128), narrow)
    sendb[...] = jnp.dot(turned, nb[:, my_cols], preferred_element_type=f32).astype(bf16)

    pl.semaphore_wait(barrier, len(greeted))
    wires = Wires(send_sem, recv_sems)

    def blk(xx, tt, step):
        return rows_all.at[
            pl.ds(pl.multiple_of((2 * step + xx) * cap, cap), cap),
            pl.ds(pl.multiple_of(tt * narrow, 128), narrow),
        ]

    def wsend(zz):
        return sendw.at[:, pl.ds(pl.multiple_of(zz * 128, 128), 128)]

    def part(ref, zz):
        return ref.at[pl.ds(pl.multiple_of(zz * cap, cap), cap), :]

    z_rows = wires.take(groups)
    to_first = wires.take(groups)
    to_second = wires.take(2 * groups)
    to_twin = wires.take(groups)

    def share_own(step):
        here = blk(x, t, step)
        src = part(sendb, z) if step == 0 else here
        wires.send(src, here, to_first + step, across)
        wires.send(src, here, to_second + 2 * step, side)
        wires.send(src, here, to_twin + step, twin)

    for step in range(1, groups):
        wires.send(part(sendb, zto(step)), blk(x, t, step), z_rows + step, peer(step, 0))
    share_own(0)
    blk(x, t, 0)[...] = part(sendb, z)[...]

    loads["xa"].wait()
    loads["ga"].wait()
    na = norm(xa_ref, ga_ref)
    heads = narrow // HD
    z_kv = wires.take(groups)
    kv_side = wires.take(1)
    q_in = wires.take(1)

    def half(xx):
        return pl.ds(pl.multiple_of(xx * cap, cap), cap)

    def project(name, ref, put):
        loads[name].wait()
        for cut in range(2):
            at = slice(cut * (narrow // 2), (cut + 1) * (narrow // 2))
            made = jnp.dot(na, ref[:, at], preferred_element_type=f32).astype(bf16)
            for sub in range(heads // 2):
                put(cut * (heads // 2) + sub, made[:, sub * HD:(sub + 1) * HD])

    def put_k(head, piece):
        kv_s[head, :, :HD] = piece

    def put_v(head, piece):
        kv_s[head, :, HD:] = piece

    def put_q(head, piece):
        q_s[head] = piece

    project("wk", wk, put_k)
    project("wv", wv, put_v)
    wires.send(kv_s.at[z], kv_all.at[e], kv_side, across)
    for step in range(1, groups):
        wires.send(kv_s.at[zto(step)], kv_all.at[e], z_kv + step, peer(step, 0))
    kv_all[e] = kv_s[z]
    project("wq", wq, put_q)
    for step in range(groups):
        for other in (0, 1):
            if step or other:
                xx = 1 - x if other else x
                wires.send(q_s.at[zto(step), half(xx), :], q_all.at[e], q_in, peer(step, other))
    q_all[e] = q_s[z, half(x), :]

    loads["rw"].wait()
    w0 = jnp.broadcast_to(rw_ref[0:1, :], (rows, rows))
    w1 = jnp.broadcast_to(rw_ref[1:2, :], (rows, rows))
    wx0 = jnp.where(odd, w1, w0)
    wx1 = jnp.where(odd, w0, w1)
    hi0 = wx0.astype(bf16).astype(f32)
    hi1 = wx1.astype(bf16).astype(f32)
    parts = jnp.where(row == 0, hi0, jnp.where(row == 1, wx0 - hi0, jnp.where(row == 2, hi1, wx1 - hi1)))
    wide = lax.broadcasted_iota(jnp.int32, (rows, groups * 128), 1).astype(f32)
    spread = jnp.where(wide == grp_f * 128 + place, 1.0, 0.0).astype(bf16)
    sendw[...] = jnp.dot(parts[:16, :].astype(bf16), spread, preferred_element_type=f32).astype(bf16)
    wt_in = wires.take(1)
    for step in range(groups):
        for other in (0, 1):
            if step or other:
                wires.send(wsend(zto(step)), wt_all.at[2 * step + x], wt_in, peer(step, other), 1)
    wt_all[x] = wsend(z)[...]

    def from_z(step):
        wires.arrived(blk(x, t, step), z_rows + step)
        share_own(step)

    def from_first(step):
        got = blk(1 - x, t, step)
        wires.arrived(got, to_first + step)
        wires.send(got, got, to_second + 2 * step + 1, side)
        wires.send(got, got, to_twin + step, twin)

    def from_second(step):
        one = blk(x, ty, step)
        wires.arrived(one, to_second + 2 * step)
        wires.send(one, one, to_twin + step, twin)

    def from_third(step):
        two = blk(1 - x, ty, step)
        wires.arrived(two, to_second + 2 * step + 1)
        wires.send(two, two, to_twin + step, twin)

    def from_twin(step):
        wires.arrived(rows_all.at[pl.ds(0, cap), :], to_twin + step)

    def pass_kv(step):
        kv_at = kv_all.at[2 * zfrom(step) + x]
        wires.arrived(kv_at, z_kv + step)
        wires.send(kv_at, kv_at, kv_side, across)

    hrows = pool
    tile = narrow // 2

    def expert_tile(h, i):
        m_at = slice(h * hrows, (h + 1) * hrows)
        n_at = slice(i * tile, (i + 1) * tile)
        g = jnp.dot(rows_all[m_at, :], gate[:, n_at], preferred_element_type=f32)
        u = jnp.dot(rows_all[m_at, :], up[:, n_at], preferred_element_type=f32)
        hid[m_at, n_at] = (g / (1.0 + jnp.exp(-g)) * u).astype(bf16)

    def down_cols(h, tt):
        m_at = slice(h * hrows, (h + 1) * hrows)
        at = pl.ds(pl.multiple_of(tt * narrow, 128), narrow)
        return jnp.dot(hid[m_at, :], down[:, at], preferred_element_type=f32) * wt_col[m_at, 0:1]

    core_at = wires.take(4)

    def give_half(h):
        for k, tt in ((1, tyc), (0, tc)):
            give[h, k] = down_cols(h, tt).astype(bf16)
            wires.send(give.at[h, k], core_in.at[h, k], core_at + 2 * h + k, twin)
        keep_f[h, 1] = down_cols(h, ty)
        keep_f[h, 0] = down_cols(h, t)

    first_at = wires.take(2 * groups)
    mid_at = wires.take(groups)
    home = wires.take(1)

    def by_side(step):
        return step % 2 == 0

    def s1_rows(step, k, xx):
        h, odd_step = step // 2, step % 2
        return s1.at[h, k, pl.ds(pl.multiple_of((2 * odd_step + xx) * cap, cap), cap), :]

    def sum_core(h):
        steps = (2 * h, 2 * h + 1)
        wires.arrived(core_in.at[h, 1], core_at + 2 * h + 1)
        s1[h, 1] = (keep_f[h, 1] + core_in[h, 1].astype(f32)).astype(bf16)
        for step in steps:
            way = side if by_side(step) else across
            wires.send(s1_rows(step, 1, 1 - x), first_in.at[step, 0], first_at + 2 * step, way)
        for step in steps:
            if by_side(step):
                wires.send(s1_rows(step, 1, x), first_in.at[step, 1], first_at + 2 * step + 1, side)
        wires.arrived(core_in.at[h, 0], core_at + 2 * h)
        s1[h, 0] = (keep_f[h, 0] + core_in[h, 0].astype(f32)).astype(bf16)
        for step in steps:
            if not by_side(step):
                wires.send(s1_rows(step, 0, 1 - x), first_in.at[step, 1], first_at + 2 * step + 1, across)

    def sum_first(step):
        wires.arrived(first_in.at[step, 0], first_at + 2 * step)
        mine = s1_rows(step, 0, 1 - x) if by_side(step) else s1_rows(step, 1, x)
        s2[step] = (mine[...].astype(f32) + first_in[step, 0].astype(f32)).astype(bf16)
        wires.send(s2.at[step], mid_in.at[step], mid_at + step, across if by_side(step) else side)

    def sum_last(step):
        wires.arrived(first_in.at[step, 1], first_at + 2 * step + 1)
        wires.arrived(mid_in.at[step], mid_at + step)
        final[step] = (
            s1_rows(step, 0, x)[...].astype(f32) + first_in[step, 1].astype(f32) + mid_in[step].astype(f32)
        ).astype(bf16)
        if step == 0:
            part(back, z)[...] = final[0]
        else:
            wires.send(final.at[step], part(back, z), home, {"ep": 2 * zfrom(step) + x, "tp": t})

    def take_weights():
        wires.arrived(wt_all.at[pl.ds(0, 2 * groups - 1)], wt_in)
        for i in range(2 * groups):
            tiles = wt_all[i].astype(f32)
            both = jnp.where(x == 0, tiles[0:1, :] + tiles[1:2, :], tiles[2:3, :] + tiles[3:4, :])
            wt_col[i * cap:(i + 1) * cap, :] = jnp.transpose(jnp.broadcast_to(both, (128, 128)))[:cap, :]

    blocks = 2 * groups
    later = jnp.where(row > lane, 1.0, 0.0).astype(bf16)
    att_in = wires.take(groups)
    att_side = wires.take(groups)
    att_twin = wires.take(1)

    def att_at(rows_at, tt, hh):
        return att.at[rows_at, pl.ds(pl.multiple_of(tt * narrow + hh * HD, HD), HD)]

    def take_kv():
        wires.arrived(kv_all.at[pl.ds(0, groups)], kv_side)
        wires.arrived(q_all.at[pl.ds(0, blocks - 1)], q_in)
        loads["off"].wait()

    def attend(kb):
        low = kb * cap
        size = blocks * cap - low
        queries = q_all[kb:, :, :].reshape(size, HD)
        scores = lax.dot_general(
            queries, kv_all[kb, :, :HD], (((1,), (1,)), ((), ())), preferred_element_type=f32
        )
        scores = scores * HD ** (-0.5) + off_ref[z]
        r_at = lax.broadcasted_iota(jnp.int32, (size, rows), 0)
        s_at = lax.broadcasted_iota(jnp.int32, (size, rows), 1)
        causal = (r_at >= cap) | (s_at < r_at + x * cap)
        keep = -(jnp.maximum(scores, 0.0) + jnp.log1p(jnp.exp(-jnp.abs(scores))))
        masked = jnp.where(causal, keep, 0.0)
        hi = masked.astype(bf16)
        lo = (masked - hi.astype(f32)).astype(bf16)
        within = jnp.dot(hi, later, preferred_element_type=f32) + jnp.dot(
            lo, later, preferred_element_type=f32
        )
        wts = jnp.where(causal, jnp.exp(scores + keep + within), 0.0).astype(bf16)
        out = jnp.dot(wts, kv_all[kb, :, HD:], preferred_element_type=f32)
        if kb:
            out = acc[low:, :] * jnp.exp(within[:, 0:1] + masked[:, 0:1]) + out
        acc[low:, :] = out
        att_s[low:low + cap, :] = out[:cap, :].astype(bf16)

        @pl.when(e == kb)
        def _():
            att_at(half(x), t, z)[...] = att_s[low:low + cap, :]

        @pl.when(e != kb)
        def _():
            wires.send(
                att_s.at[low:low + cap, :], att_at(half(x), t, z), att_in + z, {"ep": kb, "tp": t}
            )

        if kb == 0:
            wires.sent_bytes -= cap * HD * 2

    def share_att(step):
        piece = att_at(slice(None), t, zfrom(step))
        like = piece if step else att_at(slice(0, cap), t, z)
        wires.arrived(like, att_in + zfrom(step))
        wires.send(piece, piece, att_side + step, side)
        wires.send(piece, piece, att_twin, twin)

    def pass_att(step):
        piece = att_at(slice(None), ty, zfrom(step))
        wires.arrived(piece, att_side + step)
        wires.send(piece, piece, att_twin, twin)

    from_first(0)
    from_z(1)
    from_second(0)
    from_z(2)
    from_first(1)
    from_z(3)
    from_third(0)
    pass_kv(1)
    from_second(1)
    from_first(2)
    pass_kv(2)
    pass_kv(3)
    from_third(1)
    from_second(2)
    from_first(3)
    take_weights()
    loads["gate"].wait()
    loads["up"].wait()
    loads["down"].wait()
    from_twin(0)
    from_twin(1)
    expert_tile(0, 0)
    from_third(2)
    from_second(3)
    expert_tile(0, 1)
    from_third(3)
    give_half(0)
    sum_core(0)
    take_kv()
    for kb in range(4):
        attend(kb)
    from_twin(2)
    from_twin(3)
    expert_tile(1, 0)
    expert_tile(1, 1)
    sum_first(0)
    sum_first(1)
    give_half(1)
    sum_core(1)
    attend(4)
    sum_last(0)
    sum_last(1)
    attend(5)
    attend(6)
    sum_first(2)
    sum_first(3)
    attend(7)
    share_att(0)
    share_att(1)
    share_att(3)
    share_att(2)
    sum_last(2)
    sum_last(3)
    pass_att(0)
    pass_att(1)
    pass_att(3)
    pass_att(2)
    loads["wo"].wait()
    wires.arrived(att.at[:, pl.ds(0, 2 * narrow)], att_twin)
    for cut in range(2):
        at = slice(cut * tile, (cut + 1) * tile)
        mix_ref[:, at] = jnp.dot(att[...], wo[:, at], preferred_element_type=f32).astype(bf16)
    wires.arrived(back.at[pl.ds(0, (groups - 1) * cap), :], home)
    exp_ref[...] = jnp.dot(pick[...], back[...], preferred_element_type=f32).astype(bf16)
    wires.drain(weights)
    wt_sent = wt_all.at[pl.ds(0, 2 * groups - 1)]
    pltpu.make_async_copy(wt_sent, wt_sent, send_sem.at[1]).wait()


def fused_on_device(
    mixer_input, mixer_gain, query_weight, key_weight, value_weight, score_offset, out_weight,
    expert_input, expert_gain, route_ids, route_weights, gate_weight, up_weight, down_weight,
):
    f32, bf16 = jnp.float32, jnp.bfloat16
    rows, width = expert_input.shape
    narrow = out_weight.shape[1]
    groups = GROUPS
    cap = rows // 2
    pool = groups * cap
    heads = narrow // HD
    ff = gate_weight.shape[2]
    hbm = pl.BlockSpec(memory_space=pltpu.HBM)
    scratch = [
        pltpu.VMEM((rows, width), bf16),
        pltpu.VMEM((1, width), f32),
        pltpu.SMEM((heads,), f32),
        pltpu.VMEM((rows, width), bf16),
        pltpu.VMEM((1, width), f32),
        pltpu.VMEM((2, rows), jnp.int32),
        pltpu.VMEM((2, rows), f32),
        pltpu.VMEM((6 * width, narrow), bf16),
        pltpu.VMEM((ff, width), bf16),
        pltpu.SemaphoreType.DMA((LOADS,)),
        pltpu.VMEM((rows, width), bf16),
        pltpu.VMEM((rows, pool), bf16),
        pltpu.VMEM((pool, narrow), bf16),
        pltpu.VMEM((16, groups * 128), bf16),
        pltpu.VMEM((2 * pool, width), bf16),
        pltpu.VMEM((2 * groups, 16, 128), bf16),
        pltpu.VMEM((2 * pool, 128), f32),
        pltpu.VMEM((heads, rows, 2 * HD), bf16),
        pltpu.VMEM((heads, rows, HD), bf16),
        pltpu.VMEM((2 * groups, rows, 2 * HD), bf16),
        pltpu.VMEM((2 * groups, cap, HD), bf16),
        pltpu.VMEM((2 * pool, HD), f32),
        pltpu.VMEM((2 * pool, HD), bf16),
        pltpu.VMEM((rows, width), bf16),
        pltpu.VMEM((2 * pool, ff), bf16),
        pltpu.VMEM((2, 2, pool, narrow), bf16),
        pltpu.VMEM((2, 2, pool, narrow), bf16),
        pltpu.VMEM((2, 2, pool, narrow), f32),
        pltpu.VMEM((2, 2, pool, narrow), bf16),
        pltpu.VMEM((groups, 2, cap, narrow), bf16),
        pltpu.VMEM((groups, cap, narrow), bf16),
        pltpu.VMEM((groups, cap, narrow), bf16),
        pltpu.VMEM((groups, cap, narrow), bf16),
        pltpu.VMEM((pool, narrow), bf16),
        pltpu.SemaphoreType.DMA((2,)),
        pltpu.SemaphoreType.DMA((WIRES,)),
    ]
    both = pl.pallas_call(
        functools.partial(fused_kernel, groups),
        out_shape=pltpu.VMEM((2, rows, narrow), bf16),
        in_specs=[hbm] * 14,
        out_specs=pl.BlockSpec(memory_space=pltpu.VMEM),
        scratch_shapes=scratch,
        compiler_params=pltpu.CompilerParams(
            collective_id=0, has_side_effects=True, vmem_limit_bytes=48 * 1024 * 1024
        ),
        name="fused",
    )(*(pltpu.with_memory_space_constraint(value, pltpu.HBM) for value in (
        mixer_input, mixer_gain.reshape(1, width), query_weight, key_weight, value_weight, score_offset,
        out_weight, expert_input, expert_gain.reshape(1, width), route_ids.T, route_weights.T,
        gate_weight, up_weight, down_weight,
    )))
    return both[0], both[1]


def fits(mesh):
    ep, tp = mesh.shape["ep"], mesh.shape["tp"]
    return ep == 2 * GROUPS and tp == 4


def solution(mesh):
    in_specs = (
        P("ep", None),
        P(),
        P(None, "tp"),
        P(None, "tp"),
        P(None, "tp"),
        P("tp"),
        P(None, "tp"),
        P("ep", None),
        P(),
        P("ep", None),
        P("ep", None),
        P("ep", None, "tp"),
        P("ep", None, "tp"),
        P("ep", "tp", None),
    )
    out_specs = (P("ep", "tp"), P("ep", "tp"))
    return jax.shard_map(
        fused_on_device if fits(mesh) else on_device, mesh=mesh, in_specs=in_specs, out_specs=out_specs, check_vma=False
    )
```
